512 devices in a mesh: tp: 512 (over z, y, x, core).
Axes of the slice: x: 4, y: 4, z: 16, core: 2. Of those that a mesh axis runs over, the one named last changes fastest.
Arguments:
- stream: bfloat16 [16384, 128], P('tp'), may hold values from -15 to 15
- norm_gain: bfloat16 [4096], replicated, may hold values from 0.099609375 to 1.8984375
- query_weight: bfloat16 [65536, 128], P('tp'), may hold values from -0.09375 to 0.09375
- key_weight: bfloat16 [65536, 128], P('tp'), may hold values from -0.09375 to 0.09375
- value_weight: bfloat16 [65536, 128], P('tp'), may hold values from -0.09375 to 0.09375
- gate_weight: bfloat16 [65536, 128], P('tp'), may hold values from -0.09375 to 0.09375
- write_weight: bfloat16 [4096, 16], replicated, may hold values from -0.09375 to 0.09375
- decay_weight: bfloat16 [4096, 16], replicated, may hold values from -0.09375 to 0.09375
- decay_rate: float32 [16], replicated, may hold values from 0.02 to 2
- head_gain: bfloat16 [128], replicated, may hold values from 0.099609375 to 1.8984375
- out_weight: bfloat16 [65536, 128], P('tp'), may hold values from -0.125 to 0.125
- state: float32 [8192, 128, 128], P('tp'), may hold values from -4 to 4
Outputs:
- stream_out: bfloat16 [16384, 128], P('tp')
- state_out: float32 [8192, 128, 128], P('tp')
The draws below stay inside these ranges and needn't reach their ends.
All inputs are finite; a program needn't handle non-finite values.
Results may differ from the reference program's by a relative error of at most 0.012.
Values may be sent and summed in bfloat16 or wider, within the bound.
No kernel may reach another device: no remote copies, remote signals or barrier semaphores. Data moves between devices by JAX's collectives and lax.ppermute only.
A program may use at most 64 MiB of HBM per device.

```python
import math
import jax
import jax.numpy as jnp
from jax import lax

D = 4096
H = 16
DK = 128
BATCH = 512
SEQ_GROUPS = 32
DG = 128
BG = 16


def draw_stream(key, part):
    key_vals, key_scales = jax.random.split(jax.random.fold_in(key, 17))
    values = jnp.clip(jax.random.normal(key_vals, (BATCH, D), jnp.float32), -5.0, 5.0)
    scales = jnp.exp(jax.random.uniform(key_scales, (D // 128,), jnp.float32, jnp.log(0.3), jnp.log(3.0)))
    whole = values * jnp.repeat(scales, 128)[None, :]
    return whole.reshape(BATCH, SEQ_GROUPS, DG).transpose(1, 0, 2).reshape(SEQ_GROUPS * BATCH, DG).astype(jnp.bfloat16)


def level_of(stream_key, shape, pieces, smallest, top_value):
    loudness, own = 1.0, jax.random.fold_in(stream_key, 6)
    for dim, parts in pieces:
        draws = jnp.exp(jax.random.uniform(jax.random.fold_in(own, dim), (parts,), jnp.float32, smallest / len(pieces), top_value / len(pieces)))
        loudness = loudness * jnp.repeat(draws, shape[dim] // parts).reshape([-1 if axis == dim else 1 for axis in range(len(shape))])
    return loudness


def noise(stream_key, shape, spread, bound, cuts=(), dtype=jnp.bfloat16):
    values = spread * jax.random.normal(stream_key, shape, jnp.float32)
    if cuts:
        values = values * level_of(stream_key, shape, cuts, -0.22, 0.18)
    return jnp.clip(values, -bound, bound).astype(dtype)


def setup_inputs(seed: int = 0) -> dict:
    key_list = jax.random.split(jax.random.key(seed), 13)
    return {
        "stream": draw_stream(jax.random.fold_in(key_list[12], 71), 0),
        "norm_gain": jnp.clip(1.0 + 0.18 * jax.random.normal(key_list[1], (D,), jnp.float32), 0.099609375, 1.8984375).astype(jnp.bfloat16),
        "query_weight": noise(key_list[2], (H * D, DK), D ** -0.5, 0.09375, ((0, 512),)),
        "key_weight": noise(key_list[3], (H * D, DK), D ** -0.5, 0.09375, ((0, 512),)),
        "value_weight": noise(key_list[4], (H * D, DK), D ** -0.5, 0.09375, ((0, 512),)),
        "gate_weight": noise(key_list[5], (H * D, DK), D ** -0.5, 0.09375, ((0, 512),)),
        "write_weight": noise(key_list[6], (D, H), D ** -0.5, 0.09375),
        "decay_weight": noise(key_list[7], (D, H), D ** -0.5, 0.09375),
        "decay_rate": jnp.clip(jnp.exp(jax.random.uniform(key_list[8], (H,), jnp.float32, math.log(0.02), math.log(2.0))), 0.02, 2.0),
        "head_gain": jnp.clip(1.0 + 0.18 * jax.random.normal(key_list[9], (DK,), jnp.float32), 0.099609375, 1.8984375).astype(jnp.bfloat16),
        "out_weight": noise(key_list[10], (H * D, DK), (H * DK) ** -0.5, 0.125, ((0, 512),)),
        "state": noise(key_list[11], (BATCH * H, DK, DK), 0.5, 4.0, ((0, 512),), jnp.float32),
    }


EPS = 1e-06

def reference(stream, norm_gain, query_weight, key_weight, value_weight, gate_weight, write_weight, decay_weight, decay_rate, head_gain, out_weight, state):
    highest = lax.Precision.HIGHEST
    stream_f = stream.reshape(SEQ_GROUPS, BATCH, DG).transpose(1, 0, 2).reshape(BATCH, D).astype(jnp.float32)
    gained = (stream_f * norm_gain.astype(jnp.float32)).astype(jnp.bfloat16)
    row_scale = lax.rsqrt(lax.optimization_barrier(jnp.mean(stream_f * stream_f, axis=-1)) + EPS)

    def logical(weight):
        return weight.reshape(SEQ_GROUPS, H, DG, DK).transpose(0, 2, 1, 3).reshape(D, H * DK)

    def project(weight):
        product = jnp.dot(gained, weight, preferred_element_type=jnp.float32)
        return (product * row_scale[:, None]).astype(jnp.bfloat16).astype(jnp.float32)
    query_raw = project(logical(query_weight)).reshape(BATCH, H, DK)
    key_raw = project(logical(key_weight)).reshape(BATCH, H, DK)
    value_vec = project(logical(value_weight)).reshape(BATCH, H, DK)
    gate_vec = project(logical(gate_weight)).reshape(BATCH, H, DK)
    write_pre = project(write_weight)
    decay_pre = project(decay_weight)
    query_vec = query_raw * lax.rsqrt(lax.optimization_barrier(jnp.sum(query_raw * query_raw, axis=-1, keepdims=True)) + EPS) * DK ** (-0.5)
    key_vec = key_raw * lax.rsqrt(lax.optimization_barrier(jnp.sum(key_raw * key_raw, axis=-1, keepdims=True)) + EPS)
    strength = jax.nn.sigmoid(write_pre)
    decay_factor = jnp.exp(-decay_rate[None, :] * jax.nn.softplus(decay_pre))
    memory = state.reshape(SEQ_GROUPS, H, BG, DK, DK).transpose(0, 2, 1, 3, 4).reshape(BATCH, H, DK, DK)
    recalled = jnp.einsum('bhdj,bhd->bhj', memory, key_vec, precision=highest)
    correction = strength[..., None] * (value_vec - decay_factor[..., None] * recalled)
    updated = decay_factor[..., None, None] * memory + key_vec[..., :, None] * correction[..., None, :]
    readout = jnp.einsum('bhdj,bhd->bhj', updated, query_vec, precision=highest)
    scaling = lax.rsqrt(lax.optimization_barrier(jnp.mean(readout * readout, axis=-1)) + EPS)
    gated_rows = (readout * head_gain.astype(jnp.float32) * jax.nn.silu(gate_vec)).astype(jnp.bfloat16)
    out_heads = out_weight.reshape(SEQ_GROUPS, H, DG, DK).transpose(1, 3, 0, 2).reshape(H, DK, D)
    head_sums = jnp.zeros((BATCH, D), jnp.float32)
    for head_index in range(H):
        term = jnp.dot(gated_rows[:, head_index], out_heads[head_index], preferred_element_type=jnp.float32)
        head_sums = head_sums + term * scaling[:, head_index, None]
    result = (stream_f + head_sums).astype(jnp.bfloat16)
    stream_out = result.reshape(BATCH, SEQ_GROUPS, DG).transpose(1, 0, 2).reshape(SEQ_GROUPS * BATCH, DG)
    state_out = updated.reshape(SEQ_GROUPS, BG, H, DK, DK).transpose(0, 2, 1, 3, 4).reshape(BATCH * H, DK, DK)
    return (stream_out, state_out)
```

```python
import jax
import jax.numpy as jnp
from jax import lax
from jax.sharding import Mesh, PartitionSpec as P

EPS = 1e-06
PAIR = 2


def per_device(
    stream,
    norm_gain,
    query_weight,
    key_weight,
    value_weight,
    gate_weight,
    write_weight,
    decay_weight,
    decay_rate,
    head_gain,
    out_weight,
    state,
):
    f32, bf16 = jnp.float32, jnp.bfloat16
    planes = lax.axis_size("z")
    heads = lax.axis_size("h")
    my_z, my_y, my_h = lax.axis_index("z"), lax.axis_index("y"), lax.axis_index("h")
    rows, cols = stream.shape
    half = rows // PAIR
    width = cols * PAIR * planes
    size = head_gain.shape[0]
    seqs = half * planes

    own = jnp.stack([query_weight, key_weight, value_weight, gate_weight, out_weight])
    other = lax.ppermute(own, "y", [(0, 1), (1, 0)])

    blocks = jnp.broadcast_to(stream.reshape(PAIR, 1, half, cols), (PAIR, heads, half, cols))
    got = lax.all_to_all(blocks.reshape(PAIR * heads, half, cols), ("y", "h"), 0, 0)
    got = got.reshape(PAIR, seqs, cols)
    first = lax.dynamic_slice_in_dim(got, my_y, 1, 0)[0]
    second = lax.dynamic_slice_in_dim(got, 1 - my_y, 1, 0)[0]
    small_w = jnp.concatenate([write_weight, decay_weight], axis=1)

    def gained_of(block, place):
        start = (my_z * PAIR + place) * cols
        gain = lax.dynamic_slice_in_dim(norm_gain, start, cols, 0).astype(f32)
        return (block.astype(f32) * gain[None, :]).astype(bf16)

    def small_of(place):
        start = (my_z * PAIR + place) * cols
        return lax.dynamic_slice_in_dim(small_w, start, cols, 0)

    first_g, second_g = gained_of(first, my_y), gained_of(second, 1 - my_y)

    def dot(a, b):
        return jnp.dot(a, b, preferred_element_type=f32)

    small = dot(first_g, small_of(my_y)) + dot(second_g, small_of(1 - my_y))
    picked = jnp.arange(2 * heads)[None, :] % heads == my_h
    small = jnp.where(picked, small, 0.0).reshape(seqs, 2, heads).sum(axis=2)
    squares = jnp.sum(got.astype(f32) ** 2, axis=(0, 2))
    small = jnp.concatenate([small, squares[:, None]], axis=1)
    small = jnp.pad(small.reshape(planes, PAIR, half // PAIR, 3), ((0, 0), (0, 0), (0, 0), (0, 61)))
    small = small.transpose(0, 2, 1, 3).reshape(planes, half // PAIR, 128).astype(bf16)
    parts = [
        (dot(first_g, own[m]) + dot(second_g, other[m])).astype(bf16).reshape(planes, half, size)
        for m in range(4)
    ]
    packed = jnp.concatenate(parts + [small], axis=1)
    summed = lax.all_to_all(packed, "z", 0, 0).astype(f32).sum(axis=0)

    tail = summed[4 * half :].reshape(half // PAIR, PAIR, 64).transpose(1, 0, 2).reshape(half, 64)
    row_scale = lax.rsqrt(tail[:, 2] / width + EPS)

    def scaled(value):
        return (value * row_scale[:, None]).astype(bf16).astype(f32)

    query_raw, key_raw, value_vec, gate_vec = [
        scaled(summed[m * half : (m + 1) * half]) for m in range(4)
    ]
    small_pre = scaled(tail[:, :2])
    query_vec = (
        query_raw
        * lax.rsqrt(jnp.sum(query_raw * query_raw, axis=-1, keepdims=True) + EPS)
        * size ** (-0.5)
    )
    key_vec = key_raw * lax.rsqrt(jnp.sum(key_raw * key_raw, axis=-1, keepdims=True) + EPS)
    strength = jax.nn.sigmoid(small_pre[:, 0])
    rate = lax.dynamic_slice_in_dim(decay_rate, my_h, 1, 0)[0]
    factor = jnp.exp(-rate * jax.nn.softplus(small_pre[:, 1]))
    recalled = jnp.sum(state * key_vec[:, :, None], axis=1)
    correction = strength[:, None] * (value_vec - factor[:, None] * recalled)
    updated = factor[:, None, None] * state + key_vec[:, :, None] * correction[:, None, :]
    readout = jnp.sum(updated * query_vec[:, :, None], axis=1)
    scaling = lax.rsqrt(jnp.mean(readout * readout, axis=1, keepdims=True) + EPS)
    gated = (scaling * readout * head_gain.astype(f32)[None, :] * jax.nn.silu(gate_vec)).astype(bf16)

    spread = jnp.broadcast_to(gated[None], (planes, half, size))
    all_gated = lax.all_to_all(spread, "z", 0, 0).reshape(seqs, size)

    def project(weight):
        return lax.dot_general(
            all_gated, weight, (((1,), (1,)), ((), ())), preferred_element_type=f32
        ).astype(bf16)

    own_out, other_out = project(own[4]), project(other[4])
    low = jnp.where(my_y == 0, own_out, other_out)
    high = jnp.where(my_y == 0, other_out, own_out)
    outs = jnp.stack([low, high]).reshape(PAIR * heads, half, cols)
    terms = lax.all_to_all(outs, ("y", "h"), 0, 0).reshape(PAIR, heads, half, cols)
    result = terms.astype(f32).sum(axis=1).reshape(rows, cols) + stream.astype(f32)
    return result.astype(bf16), updated


def solution(mesh):
    heads = 16
    grid = Mesh(mesh.devices.reshape(-1, PAIR, heads), ("z", "y", "h"))
    every = ("z", "y", "h")
    flat, cube, same = P(every, None), P(every, None, None), P()
    placed = (flat, same, flat, flat, flat, flat, same, same, same, same, flat, cube)
    return jax.shard_map(
        per_device, mesh=grid, in_specs=placed, out_specs=(flat, cube), check_vma=False
    )
```

```python
import jax
import jax.numpy as jnp
from jax import lax
from jax.experimental import pallas as pl
from jax.experimental.pallas import tpu as pltpu
from jax.sharding import Mesh, PartitionSpec as P

EPS = 1e-06
PAIR = 2
PARTS = 4
f32, bf16 = jnp.float32, jnp.bfloat16


def row_of(values, index):
    here = lax.broadcasted_iota(jnp.int32, values.shape, 0) == index
    return jnp.sum(jnp.where(here, values, 0.0), axis=0, keepdims=True)


def dot_t(a, b):
    return lax.dot_general(a, b, (((1,), (1,)), ((), ())), preferred_element_type=f32)


def stage_kernel(
    x_hbm, gain_hbm, write_hbm, decay_hbm, rate_hbm, head_gain_hbm, *refs
):
    weights, (blocks_ref, own_ref, x_ref, misc_ref), scratch = refs[:5], refs[5:9], refs[9:]
    gain_ref, write_ref, decay_ref, rate_ref, head_gain_ref, sems = scratch
    half = blocks_ref.shape[1]
    heads = blocks_ref.shape[0] // PAIR
    cols = blocks_ref.shape[2]
    my_z, my_y, my_h = lax.axis_index("z"), lax.axis_index("y"), lax.axis_index("h")
    here = pl.ds(pl.multiple_of(my_z * (PAIR * cols), PAIR * cols), PAIR * cols)
    moves = [(x_hbm, x_ref)] + [(ref, own_ref.at[m]) for m, ref in enumerate(weights)]
    moves += [
        (gain_hbm, gain_ref),
        (write_hbm.at[:, here], write_ref),
        (decay_hbm.at[:, here], decay_ref),
        (rate_hbm, rate_ref),
        (head_gain_hbm, head_gain_ref),
    ]
    copies = [pltpu.make_async_copy(a, b, sems.at[i]) for i, (a, b) in enumerate(moves)]
    for copy in copies:
        copy.start()
    copies[0].wait()
    for place in range(PAIR):
        rows = x_ref[place * half : (place + 1) * half, :]
        for head in range(heads):
            blocks_ref[place * heads + head] = rows
    for copy in copies[1:]:
        copy.wait()
    gains = gain_ref[...].astype(f32)
    lines = [row_of(gains, my_z * PAIR + place) for place in (my_y, 1 - my_y)]
    lines.append(head_gain_ref[...].astype(f32))
    rates = rate_ref[...]
    lane = lax.broadcasted_iota(jnp.int32, rates.shape, 1)
    rate = jnp.sum(jnp.where(lane == my_h, rates, 0.0), axis=1, keepdims=True)
    lines.append(jnp.broadcast_to(rate, (1, cols)))
    for ref in (write_ref, decay_ref):
        row = row_of(ref[...].astype(f32), my_h)
        low, high = row[:, :cols], row[:, cols:]
        lines.append(jnp.where(my_y == 0, low, high))
        lines.append(jnp.where(my_y == 0, high, low))
    for i, line in enumerate(lines):
        misc_ref[i : i + 1, :] = line


def project_kernel(got_ref, own_ref, other_ref, misc_ref, packed_ref):
    planes, half = packed_ref.shape[0], got_ref.shape[1]
    cols = got_ref.shape[2]
    heads = got_ref.shape[0] // PAIR
    seqs = heads * half
    my_y = lax.axis_index("y")
    squares, gained, small = None, [], None
    for i, place in enumerate((my_y, 1 - my_y)):
        x = got_ref[pl.ds(place * heads, heads)].reshape(seqs, cols).astype(f32)
        g = (x * misc_ref[i : i + 1, :]).astype(bf16)
        gained.append(g)
        squares = x * x if squares is None else squares + x * x
        line = lax.broadcasted_iota(jnp.int32, (128, cols), 0)
        write_row, decay_row = misc_ref[4 + i : 5 + i, :], misc_ref[6 + i : 7 + i, :]
        rows = jnp.where(line == 0, write_row, jnp.where(line == 1, decay_row, 0.0)).astype(bf16)
        term = dot_t(g, rows)
        small = term if small is None else small + term
    for m in range(PARTS):
        part = jnp.dot(gained[0], own_ref[m], preferred_element_type=f32)
        part = part + jnp.dot(gained[1], other_ref[m], preferred_element_type=f32)
        packed_ref[:, m * half : (m + 1) * half, :] = part.astype(bf16).reshape(planes, half, -1)
    total = jnp.sum(squares, axis=1, keepdims=True)
    lane = lax.broadcasted_iota(jnp.int32, small.shape, 1)
    small = jnp.where(lane == 2, total, small).reshape(planes, PAIR, half // PAIR, 128)
    tail = small[:, 0] + pltpu.roll(small[:, 1].reshape(-1, 128), 64, 1).reshape(planes, -1, 128)
    packed_ref[:, PARTS * half :, :] = tail.astype(bf16)


def state_kernel(width, recv_ref, state_ref, misc_ref, spread_ref, updated_ref):
    planes, half, size = spread_ref.shape
    summed = recv_ref[0].astype(f32)
    for z in range(1, planes):
        summed = summed + recv_ref[z].astype(f32)
    tail = summed[PARTS * half :]
    tail = jnp.concatenate([tail, pltpu.roll(tail, 64, 1)], axis=0)
    row_scale = lax.rsqrt(tail[:, 2:3] / width + EPS)

    def scaled(value):
        return (value * row_scale).astype(bf16).astype(f32)

    query, key, value, gate = [scaled(summed[m * half : (m + 1) * half]) for m in range(PARTS)]
    pre = scaled(tail)
    query = query * lax.rsqrt(jnp.sum(query * query, axis=1, keepdims=True) + EPS) * size**-0.5
    key = key * lax.rsqrt(jnp.sum(key * key, axis=1, keepdims=True) + EPS)
    strength = jax.nn.sigmoid(pre[:, 0:1])
    rate = misc_ref[3:4, 0:1]
    decay_pre = pre[:, 1:2]
    softplus = jnp.maximum(decay_pre, 0.0) + jnp.log1p(jnp.exp(-jnp.abs(decay_pre)))
    factor = jnp.broadcast_to(jnp.exp(-rate * softplus), (half, size))
    query_t, key_t = query.T, key.T
    match = jnp.sum(query * key, axis=1, keepdims=True)
    readouts = []
    for b in range(half):
        memory = state_ref[b]
        key_col = jnp.broadcast_to(key_t[:, b : b + 1], (size, size))
        query_col = jnp.broadcast_to(query_t[:, b : b + 1], (size, size))
        recalled = jnp.sum(memory * key_col, axis=0, keepdims=True)
        asked = jnp.sum(memory * query_col, axis=0, keepdims=True)
        fade = factor[b : b + 1]
        correction = strength[b : b + 1] * (value[b : b + 1] - fade * recalled)
        updated_ref[b] = fade * memory + key_col * correction
        readouts.append(fade * asked + match[b : b + 1] * correction)
    readout = jnp.concatenate(readouts, axis=0)
    scaling = lax.rsqrt(jnp.mean(readout * readout, axis=1, keepdims=True) + EPS)
    silu = gate / (1.0 + jnp.exp(-gate))
    gated = (scaling * readout * misc_ref[2:3, :] * silu).astype(bf16)
    for z in range(planes):
        spread_ref[z] = gated


def output_kernel(gated_ref, own_ref, other_ref, outs_ref):
    planes, half, size = gated_ref.shape
    my_y = lax.axis_index("y")
    gated = gated_ref[...].reshape(planes * half, size)
    for place, ref in ((my_y, own_ref), (1 - my_y, other_ref)):
        term = dot_t(gated, ref[PARTS]).astype(bf16)
        outs_ref[pl.ds(place * planes, planes)] = term.reshape(planes, half, -1)


def final_kernel(terms_ref, x_ref, updated_ref, out_ref, state_hbm, sem):
    half = terms_ref.shape[1]
    heads = terms_ref.shape[0] // PAIR
    copy = pltpu.make_async_copy(updated_ref, state_hbm, sem)
    copy.start()
    for place in range(PAIR):
        where = slice(place * half, (place + 1) * half)
        total = x_ref[where, :].astype(f32)
        for head in range(heads):
            total = total + terms_ref[place * heads + head].astype(f32)
        out_ref[where, :] = total.astype(bf16)
    copy.wait()


def per_device(
    stream,
    norm_gain,
    query_weight,
    key_weight,
    value_weight,
    gate_weight,
    write_weight,
    decay_weight,
    decay_rate,
    head_gain,
    out_weight,
    state,
):
    planes = lax.axis_size("z")
    heads = lax.axis_size("h")
    rows, cols = stream.shape
    half = rows // PAIR
    size = head_gain.shape[0]
    vmem, anywhere = pl.BlockSpec(memory_space=pltpu.VMEM), pl.BlockSpec(memory_space=pl.ANY)
    kept, plain = pltpu.VMEM, jax.ShapeDtypeStruct

    def call(kernel, outs, *args):
        args = [pltpu.with_memory_space_constraint(arg, pltpu.VMEM) for arg in args]
        specs = jax.tree.map(lambda _: vmem, outs)
        return pl.pallas_call(
            kernel, out_shape=outs, in_specs=[vmem] * len(args), out_specs=specs
        )(*args)

    whole = (norm_gain.reshape(-1, cols), write_weight.T, decay_weight.T)
    whole += (decay_rate.reshape(1, -1), head_gain.reshape(1, -1))
    blocks, own, x, misc = pl.pallas_call(
        stage_kernel,
        out_shape=(
            kept((PAIR * heads, half, cols), bf16),
            kept((PARTS + 1, cols, size), bf16),
            kept((rows, cols), bf16),
            kept((8, cols), f32),
        ),
        in_specs=[anywhere] * 11,
        out_specs=(vmem,) * 4,
        scratch_shapes=[
            pltpu.VMEM(whole[0].shape, bf16),
            pltpu.VMEM((heads, PAIR * cols), bf16),
            pltpu.VMEM((heads, PAIR * cols), bf16),
            pltpu.VMEM(whole[3].shape, f32),
            pltpu.VMEM(whole[4].shape, bf16),
            pltpu.SemaphoreType.DMA((11,)),
        ],
    )(stream, *whole, query_weight, key_weight, value_weight, gate_weight, out_weight)
    other = lax.ppermute(own, "y", [(0, 1), (1, 0)])
    got = lax.all_to_all(blocks, ("y", "h"), 0, 0)
    packed = call(
        project_kernel,
        kept((planes, PARTS * half + half // PAIR, size), bf16),
        got, own, other, misc,
    )
    recv = lax.all_to_all(packed, "z", 0, 0)
    spread, updated = call(
        lambda *refs: state_kernel(cols * PAIR * planes, *refs),
        (kept((planes, half, size), bf16), kept(state.shape, f32)),
        recv, state, misc,
    )
    all_gated = lax.all_to_all(spread, "z", 0, 0)
    outs = call(output_kernel, kept((PAIR * planes, half, cols), bf16), all_gated, own, other)
    terms = lax.all_to_all(outs, ("y", "h"), 0, 0)
    last = [pltpu.with_memory_space_constraint(arg, pltpu.VMEM) for arg in (terms, x, updated)]
    return tuple(
        pl.pallas_call(
            final_kernel,
            out_shape=(plain((rows, cols), bf16), plain(state.shape, f32)),
            in_specs=[vmem] * 3,
            out_specs=(vmem, anywhere),
            scratch_shapes=[pltpu.SemaphoreType.DMA],
        )(*last)
    )


def solution(mesh):
    heads = 16
    grid = Mesh(mesh.devices.reshape(-1, PAIR, heads), ("z", "y", "h"))
    every = ("z", "y", "h")
    flat, cube, same = P(every, None), P(every, None, None), P()
    placed = (flat, same, flat, flat, flat, flat, same, same, same, same, flat, cube)
    return jax.shard_map(
        per_device, mesh=grid, in_specs=placed, out_specs=(flat, cube), check_vma=False
    )
```

```python
import jax
import jax.numpy as jnp
from jax import lax
from jax.experimental import pallas as pl
from jax.experimental.pallas import tpu as pltpu
from jax.sharding import Mesh, PartitionSpec as P


EPS = 1e-06
PAIR = 2
PARTS = 4
KEPT = 2
f32, bf16 = jnp.float32, jnp.bfloat16


def row_of(values, index):
    here = lax.broadcasted_iota(jnp.int32, values.shape, 0) == index
    return jnp.sum(jnp.where(here, values, 0.0), axis=0, keepdims=True)


def dot_t(a, b):
    return lax.dot_general(a, b, (((1,), (1,)), ((), ())), preferred_element_type=f32)


def stage_kernel(
    x_hbm, gain_hbm, write_hbm, decay_hbm, rate_hbm, head_gain_hbm, *refs
):
    weights, (blocks_hbm, own_ref, x_ref, misc_ref), scratch = refs[:5], refs[5:9], refs[9:]
    half_ref, gain_ref, write_ref, decay_ref, rate_ref, head_gain_ref, sems = scratch
    half = blocks_hbm.shape[1]
    heads = blocks_hbm.shape[0] // (2 * PAIR)
    cols = blocks_hbm.shape[2]
    my_zh, my_za = lax.axis_index("zh"), lax.axis_index("za")
    my_z, my_y, my_h = my_zh * 2 + my_za, lax.axis_index("y"), lax.axis_index("h")
    here = pl.ds(pl.multiple_of(my_z * (PAIR * cols), PAIR * cols), PAIR * cols)
    moves = [(x_hbm, x_ref)] + [(ref, own_ref.at[m]) for m, ref in enumerate(weights)]
    moves += [
        (gain_hbm, gain_ref),
        (write_hbm.at[:, here], write_ref),
        (decay_hbm.at[:, here], decay_ref),
        (rate_hbm, rate_ref),
        (head_gain_hbm, head_gain_ref),
    ]
    copies = [pltpu.make_async_copy(a, b, sems.at[i]) for i, (a, b) in enumerate(moves)]
    for copy in copies:
        copy.start()
    copies[0].wait()
    for place in range(PAIR):
        rows = x_ref[place * half : (place + 1) * half, :]
        for head in range(heads):
            half_ref[place * heads + head] = rows
    spreads = [
        pltpu.make_async_copy(
            half_ref,
            blocks_hbm.at[pl.ds(plane * PAIR * heads, PAIR * heads)],
            sems.at[len(moves) + plane],
        )
        for plane in range(2)
    ]
    for copy in spreads:
        copy.start()
    for copy in copies[1:]:
        copy.wait()
    gains = gain_ref[...].astype(f32)
    lines = [
        row_of(gains, (my_zh * 2 + plane) * PAIR + place)
        for plane in (my_za, 1 - my_za)
        for place in (my_y, 1 - my_y)
    ]
    lines.append(head_gain_ref[...].astype(f32))
    rates = rate_ref[...]
    lane = lax.broadcasted_iota(jnp.int32, rates.shape, 1)
    rate = jnp.sum(jnp.where(lane == my_h, rates, 0.0), axis=1, keepdims=True)
    lines.append(jnp.broadcast_to(rate, (1, cols)))
    for ref in (write_ref, decay_ref):
        row = row_of(ref[...].astype(f32), my_h)
        low, high = row[:, :cols], row[:, cols:]
        lines.append(jnp.where(my_y == 0, low, high))
        lines.append(jnp.where(my_y == 0, high, low))
    for i, line in enumerate(lines):
        misc_ref[i : i + 1, :] = line
    for copy in spreads:
        copy.wait()


def send_kernel(own_ref, other_ref, far_ref):
    theirs = (1 - lax.axis_index("za")) * KEPT
    for i, ref in enumerate((own_ref, other_ref)):
        for m in range(KEPT):
            far_ref[i * KEPT + m] = ref[theirs + m]


def load_kernel(state_hbm, state_ref, sem):
    copy = pltpu.make_async_copy(state_hbm, state_ref, sem)
    copy.start()
    copy.wait()


def project_kernel(got_ref, own_ref, other_ref, far_ref, misc_ref, packed_ref):
    planes, half = packed_ref.shape[0], got_ref.shape[1]
    cols = got_ref.shape[2]
    heads = got_ref.shape[0] // (2 * PAIR)
    seqs = heads * half
    my_za, my_y = lax.axis_index("za"), lax.axis_index("y")
    squares, gained, small = None, [], None
    for p, plane in enumerate((my_za, 1 - my_za)):
        for i, place in enumerate((my_y, 1 - my_y)):
            x = got_ref[pl.ds((plane * PAIR + place) * heads, heads)]
            x = x.reshape(seqs, cols).astype(f32)
            line = p * PAIR + i
            g = (x * misc_ref[line : line + 1, :]).astype(bf16)
            gained.append(g)
            if p:
                continue
            squares = x * x if squares is None else squares + x * x
            line = lax.broadcasted_iota(jnp.int32, (128, cols), 0)
            write_row, decay_row = misc_ref[6 + i : 7 + i, :], misc_ref[8 + i : 9 + i, :]
            rows = jnp.where(line == 0, write_row, jnp.where(line == 1, decay_row, 0.0))
            term = dot_t(g, rows.astype(bf16))
            small = term if small is None else small + term
    for m in range(KEPT):
        mine = my_za * KEPT + m
        weights = (own_ref[mine], other_ref[mine], far_ref[m], far_ref[KEPT + m])
        part = None
        for g, weight in zip(gained, weights):
            term = jnp.dot(g, weight, preferred_element_type=f32)
            part = term if part is None else part + term
        packed_ref[:, m * half : (m + 1) * half, :] = part.astype(bf16).reshape(planes, half, -1)
    total = jnp.sum(squares, axis=1, keepdims=True)
    lane = lax.broadcasted_iota(jnp.int32, small.shape, 1)
    small = jnp.where(lane == 2, total, small).reshape(planes, PAIR, half // PAIR, 128)
    tail = small[:, 0] + pltpu.roll(small[:, 1].reshape(-1, 128), 64, 1).reshape(planes, -1, 128)
    packed_ref[:, KEPT * half :, :] = tail.astype(bf16)


def state_kernel(width, recv_ref, state_ref, misc_ref, spread_ref, updated_ref):
    planes, half, size = spread_ref.shape
    sums = [recv_ref[0].astype(f32), recv_ref[1].astype(f32)]
    for z in range(2, planes):
        sums[z % 2] = sums[z % 2] + recv_ref[z].astype(f32)
    tail = sums[0][KEPT * half :] + sums[1][KEPT * half :]
    tail = jnp.concatenate([tail, pltpu.roll(tail, 64, 1)], axis=0)
    row_scale = lax.rsqrt(tail[:, 2:3] / width + EPS)

    def scaled(value):
        return (value * row_scale).astype(bf16).astype(f32)

    query, key, value, gate = [
        scaled(sums[p][m * half : (m + 1) * half]) for p in range(2) for m in range(KEPT)
    ]
    pre = scaled(tail)
    query = query * lax.rsqrt(jnp.sum(query * query, axis=1, keepdims=True) + EPS) * size**-0.5
    key = key * lax.rsqrt(jnp.sum(key * key, axis=1, keepdims=True) + EPS)
    strength = jax.nn.sigmoid(pre[:, 0:1])
    rate = misc_ref[5:6, 0:1]
    decay_pre = pre[:, 1:2]
    softplus = jnp.maximum(decay_pre, 0.0) + jnp.log1p(jnp.exp(-jnp.abs(decay_pre)))
    factor = jnp.broadcast_to(jnp.exp(-rate * softplus), (half, size))
    query_t, key_t = query.T, key.T
    match = jnp.sum(query * key, axis=1, keepdims=True)
    recalls, asks = [], []
    for b in range(half):
        memory = state_ref[b]
        key_col = jnp.broadcast_to(key_t[:, b : b + 1], (size, size))
        query_col = jnp.broadcast_to(query_t[:, b : b + 1], (size, size))
        recalls.append(jnp.sum(memory * key_col, axis=0, keepdims=True))
        asks.append(jnp.sum(memory * query_col, axis=0, keepdims=True))
    recalled, asked = jnp.concatenate(recalls, axis=0), jnp.concatenate(asks, axis=0)
    correction = strength * (value - factor * recalled)
    readout = factor * asked + match * correction
    for b in range(half):
        key_col = jnp.broadcast_to(key_t[:, b : b + 1], (size, size))
        updated_ref[b] = factor[b : b + 1] * state_ref[b] + key_col * correction[b : b + 1]
    scaling = lax.rsqrt(jnp.mean(readout * readout, axis=1, keepdims=True) + EPS)
    silu = gate / (1.0 + jnp.exp(-gate))
    gated = (scaling * readout * misc_ref[4:5, :] * silu).astype(bf16)
    for z in range(planes):
        spread_ref[z] = gated


def output_kernel(gated_ref, own_ref, other_ref, outs_ref):
    planes, half, size = gated_ref.shape
    my_y = lax.axis_index("y")
    gated = gated_ref[...].reshape(planes * half, size)
    for place, ref in ((my_y, own_ref), (1 - my_y, other_ref)):
        term = dot_t(gated, ref[PARTS]).astype(bf16)
        outs_ref[pl.ds(place * planes, planes)] = term.reshape(planes, half, -1)


def final_kernel(terms_ref, x_ref, updated_ref, out_hbm, state_hbm, out_ref, sems):
    half = terms_ref.shape[1]
    heads = terms_ref.shape[0] // PAIR
    state_copy = pltpu.make_async_copy(updated_ref, state_hbm, sems.at[0])
    state_copy.start()
    for place in range(PAIR):
        where = slice(place * half, (place + 1) * half)
        total = x_ref[where, :].astype(f32)
        for head in range(heads):
            total = total + terms_ref[place * heads + head].astype(f32)
        out_ref[where, :] = total.astype(bf16)
    out_copy = pltpu.make_async_copy(out_ref, out_hbm, sems.at[1])
    out_copy.start()
    state_copy.wait()
    out_copy.wait()


def per_device(
    stream,
    norm_gain,
    query_weight,
    key_weight,
    value_weight,
    gate_weight,
    write_weight,
    decay_weight,
    decay_rate,
    head_gain,
    out_weight,
    state,
):
    planes = lax.axis_size(("zh", "za"))
    heads = lax.axis_size("h")
    rows, cols = stream.shape
    half = rows // PAIR
    size = head_gain.shape[0]
    vmem, anywhere = pl.BlockSpec(memory_space=pltpu.VMEM), pl.BlockSpec(memory_space=pl.ANY)
    kept, plain = pltpu.VMEM, jax.ShapeDtypeStruct

    def call(kernel, outs, *args):
        args = [pltpu.with_memory_space_constraint(arg, pltpu.VMEM) for arg in args]
        specs = jax.tree.map(lambda _: vmem, outs)
        return pl.pallas_call(
            kernel, out_shape=outs, in_specs=[vmem] * len(args), out_specs=specs
        )(*args)

    whole = (norm_gain.reshape(-1, cols), write_weight.T, decay_weight.T)
    whole += (decay_rate.reshape(1, -1), head_gain.reshape(1, -1))
    blocks, own, x, misc = pl.pallas_call(
        stage_kernel,
        out_shape=(
            plain((2 * PAIR * heads, half, cols), bf16),
            kept((PARTS + 1, cols, size), bf16),
            kept((rows, cols), bf16),
            kept((16, cols), f32),
        ),
        in_specs=[anywhere] * 11,
        out_specs=(anywhere, vmem, vmem, vmem),
        scratch_shapes=[
            pltpu.VMEM((PAIR * heads, half, cols), bf16),
            pltpu.VMEM(whole[0].shape, bf16),
            pltpu.VMEM((heads, PAIR * cols), bf16),
            pltpu.VMEM((heads, PAIR * cols), bf16),
            pltpu.VMEM(whole[3].shape, f32),
            pltpu.VMEM(whole[4].shape, bf16),
            pltpu.SemaphoreType.DMA((13,)),
        ],
    )(stream, *whole, query_weight, key_weight, value_weight, gate_weight, out_weight)
    other = lax.ppermute(own, "y", [(0, 1), (1, 0)])
    far = call(send_kernel, kept((PAIR * KEPT, cols, size), bf16), own, other)
    far = lax.ppermute(far, "za", [(0, 1), (1, 0)])
    memory = pl.pallas_call(
        load_kernel,
        out_shape=kept(state.shape, f32),
        in_specs=[anywhere],
        out_specs=vmem,
        scratch_shapes=[pltpu.SemaphoreType.DMA],
    )(state)
    got = lax.all_to_all(blocks, ("za", "y", "h"), 0, 0)
    packed = call(
        project_kernel,
        kept((planes, KEPT * half + half // PAIR, size), bf16),
        got, own, other, far, misc,
    )
    recv = lax.all_to_all(packed, ("zh", "za"), 0, 0)
    spread, updated = call(
        lambda *refs: state_kernel(cols * PAIR * planes, *refs),
        (kept((planes, half, size), bf16), kept(state.shape, f32)),
        recv, memory, misc,
    )
    all_gated = lax.all_to_all(spread, ("zh", "za"), 0, 0)
    outs = call(output_kernel, kept((PAIR * planes, half, cols), bf16), all_gated, own, other)
    terms = lax.all_to_all(outs, ("y", "h"), 0, 0)
    last = [pltpu.with_memory_space_constraint(arg, pltpu.VMEM) for arg in (terms, x, updated)]
    return tuple(
        pl.pallas_call(
            final_kernel,
            out_shape=(plain((rows, cols), bf16), plain(state.shape, f32)),
            in_specs=[vmem] * 3,
            out_specs=(anywhere, anywhere),
            scratch_shapes=[pltpu.VMEM((rows, cols), bf16), pltpu.SemaphoreType.DMA((2,))],
        )(*last)
    )


def solution(mesh):
    heads = 16
    grid = Mesh(mesh.devices.reshape(-1, 2, PAIR, heads), ("zh", "za", "y", "h"))
    every = ("zh", "za", "y", "h")
    flat, cube, same = P(every, None), P(every, None, None), P()
    placed = (flat, same, flat, flat, flat, flat, same, same, same, same, flat, cube)
    return jax.shard_map(
        per_device, mesh=grid, in_specs=placed, out_specs=(flat, cube), check_vma=False
    )
```

```python
import jax
import jax.numpy as jnp
from jax import lax
from jax.experimental import pallas as pl
from jax.experimental.pallas import tpu as pltpu
from jax.sharding import Mesh, PartitionSpec as P


EPS = 1e-06
PAIR = 2
PARTS = 4
KEPT = 2
f32, bf16 = jnp.float32, jnp.bfloat16


def row_of(values, index):
    here = lax.broadcasted_iota(jnp.int32, values.shape, 0) == index
    return jnp.sum(jnp.where(here, values, 0.0), axis=0, keepdims=True)


def dot_t(a, b):
    return lax.dot_general(a, b, (((1,), (1,)), ((), ())), preferred_element_type=f32)


def stage_kernel(
    x_hbm, gain_hbm, write_hbm, decay_hbm, rate_hbm, head_gain_hbm, *refs
):
    weights, (blocks_hbm, own_ref, x_ref, misc_ref), scratch = refs[:5], refs[5:9], refs[9:]
    half_ref, gain_ref, write_ref, decay_ref, rate_ref, head_gain_ref, sems = scratch
    half = blocks_hbm.shape[1]
    heads = blocks_hbm.shape[0] // (2 * PAIR)
    cols = blocks_hbm.shape[2]
    my_zh, my_za = lax.axis_index("zh"), lax.axis_index("za")
    my_z, my_y, my_h = my_zh * 2 + my_za, lax.axis_index("y"), lax.axis_index("h")
    here = pl.ds(pl.multiple_of(my_z * (PAIR * cols), PAIR * cols), PAIR * cols)
    moves = [(x_hbm, x_ref)] + [(ref, own_ref.at[m]) for m, ref in enumerate(weights)]
    moves += [
        (gain_hbm, gain_ref),
        (write_hbm.at[:, here], write_ref),
        (decay_hbm.at[:, here], decay_ref),
        (rate_hbm, rate_ref),
        (head_gain_hbm, head_gain_ref),
    ]
    copies = [pltpu.make_async_copy(a, b, sems.at[i]) for i, (a, b) in enumerate(moves)]
    for copy in copies:
        copy.start()
    copies[0].wait()
    for place in range(PAIR):
        rows = x_ref[place * half : (place + 1) * half, :]
        for head in range(heads):
            half_ref[place * heads + head] = rows
    spreads = [
        pltpu.make_async_copy(
            half_ref,
            blocks_hbm.at[pl.ds(plane * PAIR * heads, PAIR * heads)],
            sems.at[len(moves) + plane],
        )
        for plane in range(2)
    ]
    for copy in spreads:
        copy.start()
    for copy in copies[1:]:
        copy.wait()
    gains = gain_ref[...].astype(f32)
    lines = [
        row_of(gains, (my_zh * 2 + plane) * PAIR + place)
        for plane in (my_za, 1 - my_za)
        for place in (my_y, 1 - my_y)
    ]
    lines.append(head_gain_ref[...].astype(f32))
    rates = rate_ref[...]
    lane = lax.broadcasted_iota(jnp.int32, rates.shape, 1)
    rate = jnp.sum(jnp.where(lane == my_h, rates, 0.0), axis=1, keepdims=True)
    lines.append(jnp.broadcast_to(rate, (1, cols)))
    for ref in (write_ref, decay_ref):
        row = row_of(ref[...].astype(f32), my_h)
        low, high = row[:, :cols], row[:, cols:]
        lines.append(jnp.where(my_y == 0, low, high))
        lines.append(jnp.where(my_y == 0, high, low))
    for i, line in enumerate(lines):
        misc_ref[i : i + 1, :] = line
    for copy in spreads:
        copy.wait()


def send_kernel(own_ref, other_ref, far_ref):
    theirs = (1 - lax.axis_index("za")) * KEPT
    for i, ref in enumerate((own_ref, other_ref)):
        for m in range(KEPT):
            far_ref[i * KEPT + m] = ref[theirs + m]


def load_kernel(state_hbm, state_ref, sem):
    copy = pltpu.make_async_copy(state_hbm, state_ref, sem)
    copy.start()
    copy.wait()


def project_kernel(got_ref, own_ref, other_ref, far_ref, misc_ref, packed_ref):
    planes, half = packed_ref.shape[0], got_ref.shape[1]
    cols = got_ref.shape[2]
    heads = got_ref.shape[0] // (2 * PAIR)
    seqs = heads * half
    my_za, my_y = lax.axis_index("za"), lax.axis_index("y")
    squares, gained, small = None, [], None
    for p, plane in enumerate((my_za, 1 - my_za)):
        for i, place in enumerate((my_y, 1 - my_y)):
            x = got_ref[pl.ds((plane * PAIR + place) * heads, heads)]
            x = x.reshape(seqs, cols).astype(f32)
            line = p * PAIR + i
            g = (x * misc_ref[line : line + 1, :]).astype(bf16)
            gained.append(g)
            if p:
                continue
            squares = x * x if squares is None else squares + x * x
            line = lax.broadcasted_iota(jnp.int32, (128, cols), 0)
            write_row, decay_row = misc_ref[6 + i : 7 + i, :], misc_ref[8 + i : 9 + i, :]
            rows = jnp.where(line == 0, write_row, jnp.where(line == 1, decay_row, 0.0))
            term = dot_t(g, rows.astype(bf16))
            small = term if small is None else small + term
    for m in range(KEPT):
        mine = my_za * KEPT + m
        weights = (own_ref[mine], other_ref[mine], far_ref[m], far_ref[KEPT + m])
        part = None
        for g, weight in zip(gained, weights):
            term = jnp.dot(g, weight, preferred_element_type=f32)
            part = term if part is None else part + term
        part = part.astype(bf16).reshape(planes, half // 2, 2, 128)
        packed_ref[:, m * half // 2 : (m + 1) * half // 2] = part
    total = jnp.sum(squares, axis=1, keepdims=True)
    lane = lax.broadcasted_iota(jnp.int32, small.shape, 1)
    small = jnp.where(lane == 2, total, small).T[:8]
    lane = lax.broadcasted_iota(jnp.int32, (1, 128), 1)
    for z in range(planes):
        start = z * half // 128 * 128
        line = small[:, start : start + 128]
        mine = lane // half == z % (128 // half)
        first = jnp.where(mine, line[0:1], pltpu.roll(line[1:2], 64, 1))
        tail = jnp.concatenate([first, line[2:3]], axis=0)
        packed_ref[z, KEPT * half // 2] = tail.astype(bf16)


def state_kernel(width, recv_ref, state_ref, misc_ref, spread_ref, updated_ref):
    planes, half, size = spread_ref.shape
    sums = [recv_ref[0].astype(f32), recv_ref[1].astype(f32)]
    for z in range(2, planes):
        sums[z % 2] = sums[z % 2] + recv_ref[z].astype(f32)
    tail = sums[0][KEPT * half // 2] + sums[1][KEPT * half // 2]
    my_z = lax.axis_index("zh") * 2 + lax.axis_index("za")
    tail = jnp.concatenate([tail, jnp.zeros((6, 128), f32)], axis=0)
    tail = pltpu.roll(tail, (128 - my_z % (128 // half) * half) % 128, 1)
    tail = jnp.concatenate([tail, pltpu.roll(tail, 64, 1)], axis=0).T[:half]
    sums = [part[: KEPT * half // 2].reshape(KEPT * half, size) for part in sums]
    row_scale = lax.rsqrt(tail[:, 1:2] / width + EPS)

    def scaled(value):
        return (value * row_scale).astype(bf16).astype(f32)

    query, key, value, gate = [
        scaled(sums[p][m * half : (m + 1) * half]) for p in range(2) for m in range(KEPT)
    ]
    pre = scaled(tail)
    query = query * lax.rsqrt(jnp.sum(query * query, axis=1, keepdims=True) + EPS) * size**-0.5
    key = key * lax.rsqrt(jnp.sum(key * key, axis=1, keepdims=True) + EPS)
    strength = jax.nn.sigmoid(pre[:, 0:1])
    rate = misc_ref[5:6, 0:1]
    decay_pre = pre[:, 8:9]
    softplus = jnp.maximum(decay_pre, 0.0) + jnp.log1p(jnp.exp(-jnp.abs(decay_pre)))
    factor = jnp.broadcast_to(jnp.exp(-rate * softplus), (half, size))
    query_t, key_t = query.T, key.T
    match = jnp.sum(query * key, axis=1, keepdims=True)
    recalls, asks = [], []
    for b in range(half):
        memory = state_ref[b]
        key_col = jnp.broadcast_to(key_t[:, b : b + 1], (size, size))
        query_col = jnp.broadcast_to(query_t[:, b : b + 1], (size, size))
        recalls.append(jnp.sum(memory * key_col, axis=0, keepdims=True))
        asks.append(jnp.sum(memory * query_col, axis=0, keepdims=True))
    recalled, asked = jnp.concatenate(recalls, axis=0), jnp.concatenate(asks, axis=0)
    correction = strength * (value - factor * recalled)
    readout = factor * asked + match * correction
    for b in range(half):
        key_col = jnp.broadcast_to(key_t[:, b : b + 1], (size, size))
        updated_ref[b] = factor[b : b + 1] * state_ref[b] + key_col * correction[b : b + 1]
    scaling = lax.rsqrt(jnp.mean(readout * readout, axis=1, keepdims=True) + EPS)
    silu = gate / (1.0 + jnp.exp(-gate))
    gated = (scaling * readout * misc_ref[4:5, :] * silu).astype(bf16)
    for z in range(planes):
        spread_ref[z] = gated


def output_kernel(gated_ref, own_ref, other_ref, outs_ref):
    planes, half, size = gated_ref.shape
    my_y = lax.axis_index("y")
    gated = gated_ref[...].reshape(planes * half, size)
    for place, ref in ((my_y, own_ref), (1 - my_y, other_ref)):
        term = dot_t(gated, ref[PARTS]).astype(bf16)
        outs_ref[pl.ds(place * planes, planes)] = term.reshape(planes, half, -1)


def final_kernel(terms_ref, x_ref, updated_ref, out_hbm, state_hbm, out_ref, sems):
    half = terms_ref.shape[1]
    heads = terms_ref.shape[0] // PAIR
    state_copy = pltpu.make_async_copy(updated_ref, state_hbm, sems.at[0])
    state_copy.start()
    for place in range(PAIR):
        where = slice(place * half, (place + 1) * half)
        total = x_ref[where, :].astype(f32)
        for head in range(heads):
            total = total + terms_ref[place * heads + head].astype(f32)
        out_ref[where, :] = total.astype(bf16)
    out_copy = pltpu.make_async_copy(out_ref, out_hbm, sems.at[1])
    out_copy.start()
    state_copy.wait()
    out_copy.wait()


def per_device(
    stream,
    norm_gain,
    query_weight,
    key_weight,
    value_weight,
    gate_weight,
    write_weight,
    decay_weight,
    decay_rate,
    head_gain,
    out_weight,
    state,
):
    planes = lax.axis_size(("zh", "za"))
    heads = lax.axis_size("h")
    rows, cols = stream.shape
    half = rows // PAIR
    size = head_gain.shape[0]
    vmem, anywhere = pl.BlockSpec(memory_space=pltpu.VMEM), pl.BlockSpec(memory_space=pl.ANY)
    kept, plain = pltpu.VMEM, jax.ShapeDtypeStruct

    def call(kernel, outs, *args):
        args = [pltpu.with_memory_space_constraint(arg, pltpu.VMEM) for arg in args]
        specs = jax.tree.map(lambda _: vmem, outs)
        return pl.pallas_call(
            kernel, out_shape=outs, in_specs=[vmem] * len(args), out_specs=specs
        )(*args)

    whole = (norm_gain.reshape(-1, cols), write_weight.T, decay_weight.T)
    whole += (decay_rate.reshape(1, -1), head_gain.reshape(1, -1))
    blocks, own, x, misc = pl.pallas_call(
        stage_kernel,
        out_shape=(
            plain((2 * PAIR * heads, half, cols), bf16),
            kept((PARTS + 1, cols, size), bf16),
            kept((rows, cols), bf16),
            kept((16, cols), f32),
        ),
        in_specs=[anywhere] * 11,
        out_specs=(anywhere, vmem, vmem, vmem),
        scratch_shapes=[
            pltpu.VMEM((PAIR * heads, half, cols), bf16),
            pltpu.VMEM(whole[0].shape, bf16),
            pltpu.VMEM((heads, PAIR * cols), bf16),
            pltpu.VMEM((heads, PAIR * cols), bf16),
            pltpu.VMEM(whole[3].shape, f32),
            pltpu.VMEM(whole[4].shape, bf16),
            pltpu.SemaphoreType.DMA((13,)),
        ],
    )(stream, *whole, query_weight, key_weight, value_weight, gate_weight, out_weight)
    other = lax.ppermute(own, "y", [(0, 1), (1, 0)])
    far = call(send_kernel, kept((PAIR * KEPT, cols, size), bf16), own, other)
    far = lax.ppermute(far, "za", [(0, 1), (1, 0)])
    memory = pl.pallas_call(
        load_kernel,
        out_shape=kept(state.shape, f32),
        in_specs=[anywhere],
        out_specs=vmem,
        scratch_shapes=[pltpu.SemaphoreType.DMA],
    )(state)
    got = lax.all_to_all(blocks, ("za", "y", "h"), 0, 0)
    packed = call(
        project_kernel,
        kept((planes, KEPT * half // 2 + 1, 2, size), bf16),
        got, own, other, far, misc,
    )
    recv = lax.all_to_all(packed, ("zh", "za"), 0, 0)
    spread, updated = call(
        lambda *refs: state_kernel(cols * PAIR * planes, *refs),
        (kept((planes, half, size), bf16), kept(state.shape, f32)),
        recv, memory, misc,
    )
    all_gated = lax.all_to_all(spread, ("zh", "za"), 0, 0)
    outs = call(output_kernel, kept((PAIR * planes, half, cols), bf16), all_gated, own, other)
    terms = lax.all_to_all(outs, ("y", "h"), 0, 0)
    last = [pltpu.with_memory_space_constraint(arg, pltpu.VMEM) for arg in (terms, x, updated)]
    return tuple(
        pl.pallas_call(
            final_kernel,
            out_shape=(plain((rows, cols), bf16), plain(state.shape, f32)),
            in_specs=[vmem] * 3,
            out_specs=(anywhere, anywhere),
            scratch_shapes=[pltpu.VMEM((rows, cols), bf16), pltpu.SemaphoreType.DMA((2,))],
        )(*last)
    )


def solution(mesh):
    heads = 16
    grid = Mesh(mesh.devices.reshape(-1, 2, PAIR, heads), ("zh", "za", "y", "h"))
    every = ("zh", "za", "y", "h")
    flat, cube, same = P(every, None), P(every, None, None), P()
    placed = (flat, same, flat, flat, flat, flat, same, same, same, same, flat, cube)
    return jax.shard_map(
        per_device, mesh=grid, in_specs=placed, out_specs=(flat, cube), check_vma=False
    )
```

```python
import jax
import jax.numpy as jnp
from jax import lax
from jax.experimental import pallas as pl
from jax.experimental.pallas import tpu as pltpu
from jax.sharding import Mesh, PartitionSpec as P


EPS = 1e-06
PAIR = 2
PARTS = 4
KEPT = 2
f32, bf16 = jnp.float32, jnp.bfloat16


def row_of(values, index):
    here = lax.broadcasted_iota(jnp.int32, values.shape, 0) == index
    return jnp.sum(jnp.where(here, values, 0.0), axis=0, keepdims=True)


def dot_t(a, b):
    return lax.dot_general(a, b, (((1,), (1,)), ((), ())), preferred_element_type=f32)


def stage_kernel(
    x_hbm, gain_hbm, write_hbm, decay_hbm, rate_hbm, head_gain_hbm, *refs
):
    weights, (blocks_hbm, own_ref, x_ref, misc_ref), scratch = refs[:5], refs[5:9], refs[9:]
    half_ref, gain_ref, write_ref, decay_ref, rate_ref, head_gain_ref, sems = scratch
    half = blocks_hbm.shape[1]
    heads = blocks_hbm.shape[0] // (2 * PAIR)
    cols = blocks_hbm.shape[2]
    my_zh, my_za = lax.axis_index("zh"), lax.axis_index("za")
    my_z, my_y, my_h = my_zh * 2 + my_za, lax.axis_index("y"), lax.axis_index("h")
    here = pl.ds(pl.multiple_of(my_z * (PAIR * cols), PAIR * cols), PAIR * cols)
    moves = [(x_hbm, x_ref)] + [(ref, own_ref.at[m]) for m, ref in enumerate(weights)]
    moves += [
        (gain_hbm, gain_ref),
        (write_hbm.at[:, here], write_ref),
        (decay_hbm.at[:, here], decay_ref),
        (rate_hbm, rate_ref),
        (head_gain_hbm, head_gain_ref),
    ]
    copies = [pltpu.make_async_copy(a, b, sems.at[i]) for i, (a, b) in enumerate(moves)]
    for copy in copies:
        copy.start()
    copies[0].wait()
    for place in range(PAIR):
        rows = x_ref[place * half : (place + 1) * half, :]
        for head in range(heads):
            half_ref[place * heads + head] = rows
    spreads = [
        pltpu.make_async_copy(
            half_ref,
            blocks_hbm.at[pl.ds(plane * PAIR * heads, PAIR * heads)],
            sems.at[len(moves) + plane],
        )
        for plane in range(2)
    ]
    for copy in spreads:
        copy.start()
    for copy in copies[1:]:
        copy.wait()
    gains = gain_ref[...].astype(f32)
    lines = [
        row_of(gains, (my_zh * 2 + plane) * PAIR + place)
        for plane in (my_za, 1 - my_za)
        for place in (my_y, 1 - my_y)
    ]
    lines.append(head_gain_ref[...].astype(f32))
    rates = rate_ref[...]
    lane = lax.broadcasted_iota(jnp.int32, rates.shape, 1)
    rate = jnp.sum(jnp.where(lane == my_h, rates, 0.0), axis=1, keepdims=True)
    lines.append(jnp.broadcast_to(rate, (1, cols)))
    for ref in (write_ref, decay_ref):
        row = row_of(ref[...].astype(f32), my_h)
        low, high = row[:, :cols], row[:, cols:]
        lines.append(jnp.where(my_y == 0, low, high))
        lines.append(jnp.where(my_y == 0, high, low))
    for i, line in enumerate(lines):
        misc_ref[i : i + 1, :] = line
    for copy in spreads:
        copy.wait()


def send_kernel(own_ref, other_ref, far_ref):
    theirs = (1 - lax.axis_index("za")) * KEPT
    for i, ref in enumerate((own_ref, other_ref)):
        for m in range(KEPT):
            far_ref[i * KEPT + m] = ref[theirs + m]


def load_kernel(state_hbm, state_ref, sem):
    copy = pltpu.make_async_copy(state_hbm, state_ref, sem)
    copy.start()
    copy.wait()


def project_kernel(got_ref, own_ref, other_ref, far_ref, misc_ref, packed_ref):
    planes, half = packed_ref.shape[0], got_ref.shape[1]
    cols = got_ref.shape[2]
    heads = got_ref.shape[0] // (2 * PAIR)
    seqs = heads * half
    my_za, my_y = lax.axis_index("za"), lax.axis_index("y")
    squares, gained, small = None, [], None
    for p, plane in enumerate((my_za, 1 - my_za)):
        for i, place in enumerate((my_y, 1 - my_y)):
            x = got_ref[pl.ds((plane * PAIR + place) * heads, heads)]
            x = x.reshape(seqs, cols).astype(f32)
            line = p * PAIR + i
            g = (x * misc_ref[line : line + 1, :]).astype(bf16)
            gained.append(g)
            if p:
                continue
            squares = x * x if squares is None else squares + x * x
            line = lax.broadcasted_iota(jnp.int32, (128, cols), 0)
            write_row, decay_row = misc_ref[6 + i : 7 + i, :], misc_ref[8 + i : 9 + i, :]
            rows = jnp.where(line == 0, write_row, jnp.where(line == 1, decay_row, 0.0))
            term = dot_t(g, rows.astype(bf16))
            small = term if small is None else small + term
    for m in range(KEPT):
        mine = my_za * KEPT + m
        weights = (own_ref[mine], other_ref[mine], far_ref[m], far_ref[KEPT + m])
        part = None
        for g, weight in zip(gained, weights):
            term = jnp.dot(g, weight, preferred_element_type=f32)
            part = term if part is None else part + term
        part = part.astype(bf16).reshape(planes, half // 2, 2, 128)
        packed_ref[:, m * half // 2 : (m + 1) * half // 2] = part
    total = jnp.sum(squares, axis=1, keepdims=True)
    lane = lax.broadcasted_iota(jnp.int32, small.shape, 1)
    small = jnp.where(lane == 2, total, small).T[:8]
    lane = lax.broadcasted_iota(jnp.int32, (1, 128), 1)
    for z in range(planes):
        start = z * half // 128 * 128
        line = small[:, start : start + 128]
        mine = lane // half == z % (128 // half)
        first = jnp.where(mine, line[0:1], pltpu.roll(line[1:2], 64, 1))
        tail = jnp.concatenate([first, line[2:3]], axis=0)
        packed_ref[z, KEPT * half // 2] = tail.astype(bf16)


def state_kernel(width, recv_ref, state_ref, misc_ref, spread_ref, updated_ref):
    planes, half, size = spread_ref.shape
    sums = [recv_ref[0].astype(f32), recv_ref[1].astype(f32)]
    for z in range(2, planes):
        sums[z % 2] = sums[z % 2] + recv_ref[z].astype(f32)
    tail = sums[0][KEPT * half // 2] + sums[1][KEPT * half // 2]
    my_z = lax.axis_index("zh") * 2 + lax.axis_index("za")
    tail = jnp.concatenate([tail, jnp.zeros((6, 128), f32)], axis=0)
    tail = pltpu.roll(tail, (128 - my_z % (128 // half) * half) % 128, 1)
    tail = jnp.concatenate([tail, pltpu.roll(tail, 64, 1)], axis=0).T[:half]
    sums = [part[: KEPT * half // 2].reshape(KEPT * half, size) for part in sums]
    row_scale = lax.rsqrt(tail[:, 1:2] / width + EPS)

    def scaled(value):
        return (value * row_scale).astype(bf16).astype(f32)

    query, key, value, gate = [
        scaled(sums[p][m * half : (m + 1) * half]) for p in range(2) for m in range(KEPT)
    ]
    pre = scaled(tail)
    query_norm = lax.rsqrt(jnp.sum(query * query, axis=1, keepdims=True) + EPS) * size**-0.5
    key_norm = lax.rsqrt(jnp.sum(key * key, axis=1, keepdims=True) + EPS)
    strength = jax.nn.sigmoid(pre[:, 0:1])
    rate = misc_ref[5:6, 0:1]
    decay_pre = pre[:, 8:9]
    softplus = jnp.maximum(decay_pre, 0.0) + jnp.log1p(jnp.exp(-jnp.abs(decay_pre)))
    factor = jnp.broadcast_to(jnp.exp(-rate * softplus), (half, size))
    query_t, key_t = query.T.astype(bf16), key.T.astype(bf16)
    match = jnp.sum(query * key, axis=1, keepdims=True) * query_norm * key_norm
    readouts = []
    for b in range(half):
        memory = state_ref[b]
        key_col = jnp.broadcast_to(key_t[:, b : b + 1], (size, size)).astype(f32)
        query_col = jnp.broadcast_to(query_t[:, b : b + 1], (size, size)).astype(f32)
        one = slice(b, b + 1)
        recalled = jnp.sum(memory * key_col, axis=0, keepdims=True) * key_norm[one]
        asked = jnp.sum(memory * query_col, axis=0, keepdims=True) * query_norm[one]
        fade = factor[one]
        correction = strength[one] * (value[one] - fade * recalled)
        updated_ref[b] = fade * memory + key_col * (key_norm[one] * correction)
        readouts.append(fade * asked + match[one] * correction)
    readout = jnp.concatenate(readouts, axis=0)
    scaling = lax.rsqrt(jnp.mean(readout * readout, axis=1, keepdims=True) + EPS)
    silu = gate / (1.0 + jnp.exp(-gate))
    gated = (scaling * readout * misc_ref[4:5, :] * silu).astype(bf16)
    for z in range(planes):
        spread_ref[z] = gated


def output_kernel(gated_ref, own_ref, other_ref, outs_ref):
    planes, half, size = gated_ref.shape
    my_y = lax.axis_index("y")
    gated = gated_ref[...].reshape(planes * half, size)
    for place, ref in ((my_y, own_ref), (1 - my_y, other_ref)):
        term = dot_t(gated, ref[PARTS]).astype(bf16)
        outs_ref[pl.ds(place * planes, planes)] = term.reshape(planes, half, -1)


def final_kernel(terms_ref, x_ref, updated_ref, out_hbm, state_hbm, out_ref, sems):
    half = terms_ref.shape[1]
    heads = terms_ref.shape[0] // PAIR
    state_copy = pltpu.make_async_copy(updated_ref, state_hbm, sems.at[0])
    state_copy.start()
    for place in range(PAIR):
        where = slice(place * half, (place + 1) * half)
        total = x_ref[where, :].astype(f32)
        for head in range(heads):
            total = total + terms_ref[place * heads + head].astype(f32)
        out_ref[where, :] = total.astype(bf16)
    out_copy = pltpu.make_async_copy(out_ref, out_hbm, sems.at[1])
    out_copy.start()
    state_copy.wait()
    out_copy.wait()


def per_device(
    stream,
    norm_gain,
    query_weight,
    key_weight,
    value_weight,
    gate_weight,
    write_weight,
    decay_weight,
    decay_rate,
    head_gain,
    out_weight,
    state,
):
    planes = lax.axis_size(("zh", "za"))
    heads = lax.axis_size("h")
    rows, cols = stream.shape
    half = rows // PAIR
    size = head_gain.shape[0]
    vmem, anywhere = pl.BlockSpec(memory_space=pltpu.VMEM), pl.BlockSpec(memory_space=pl.ANY)
    kept, plain = pltpu.VMEM, jax.ShapeDtypeStruct

    def call(kernel, outs, *args):
        args = [pltpu.with_memory_space_constraint(arg, pltpu.VMEM) for arg in args]
        specs = jax.tree.map(lambda _: vmem, outs)
        return pl.pallas_call(
            kernel, out_shape=outs, in_specs=[vmem] * len(args), out_specs=specs
        )(*args)

    whole = (norm_gain.reshape(-1, cols), write_weight.T, decay_weight.T)
    whole += (decay_rate.reshape(1, -1), head_gain.reshape(1, -1))
    blocks, own, x, misc = pl.pallas_call(
        stage_kernel,
        out_shape=(
            plain((2 * PAIR * heads, half, cols), bf16),
            kept((PARTS + 1, cols, size), bf16),
            kept((rows, cols), bf16),
            kept((16, cols), f32),
        ),
        in_specs=[anywhere] * 11,
        out_specs=(anywhere, vmem, vmem, vmem),
        scratch_shapes=[
            pltpu.VMEM((PAIR * heads, half, cols), bf16),
            pltpu.VMEM(whole[0].shape, bf16),
            pltpu.VMEM((heads, PAIR * cols), bf16),
            pltpu.VMEM((heads, PAIR * cols), bf16),
            pltpu.VMEM(whole[3].shape, f32),
            pltpu.VMEM(whole[4].shape, bf16),
            pltpu.SemaphoreType.DMA((13,)),
        ],
    )(stream, *whole, query_weight, key_weight, value_weight, gate_weight, out_weight)
    other = lax.ppermute(own, "y", [(0, 1), (1, 0)])
    far = call(send_kernel, kept((PAIR * KEPT, cols, size), bf16), own, other)
    far = lax.ppermute(far, "za", [(0, 1), (1, 0)])
    memory = pl.pallas_call(
        load_kernel,
        out_shape=kept(state.shape, f32),
        in_specs=[anywhere],
        out_specs=vmem,
        scratch_shapes=[pltpu.SemaphoreType.DMA],
    )(state)
    got = lax.all_to_all(blocks, ("za", "y", "h"), 0, 0)
    packed = call(
        project_kernel,
        kept((planes, KEPT * half // 2 + 1, 2, size), bf16),
        got, own, other, far, misc,
    )
    recv = lax.all_to_all(packed, ("zh", "za"), 0, 0)
    spread, updated = call(
        lambda *refs: state_kernel(cols * PAIR * planes, *refs),
        (kept((planes, half, size), bf16), kept(state.shape, f32)),
        recv, memory, misc,
    )
    all_gated = lax.all_to_all(spread, ("zh", "za"), 0, 0)
    outs = call(output_kernel, kept((PAIR * planes, half, cols), bf16), all_gated, own, other)
    terms = lax.all_to_all(outs, ("y", "h"), 0, 0)
    last = [pltpu.with_memory_space_constraint(arg, pltpu.VMEM) for arg in (terms, x, updated)]
    return tuple(
        pl.pallas_call(
            final_kernel,
            out_shape=(plain((rows, cols), bf16), plain(state.shape, f32)),
            in_specs=[vmem] * 3,
            out_specs=(anywhere, anywhere),
            scratch_shapes=[pltpu.VMEM((rows, cols), bf16), pltpu.SemaphoreType.DMA((2,))],
        )(*last)
    )


def solution(mesh):
    heads = 16
    grid = Mesh(mesh.devices.reshape(-1, 2, PAIR, heads), ("zh", "za", "y", "h"))
    every = ("zh", "za", "y", "h")
    flat, cube, same = P(every, None), P(every, None, None), P()
    placed = (flat, same, flat, flat, flat, flat, same, same, same, same, flat, cube)
    return jax.shard_map(
        per_device, mesh=grid, in_specs=placed, out_specs=(flat, cube), check_vma=False
    )
```

```python
import jax
import jax.numpy as jnp
from jax import lax
from jax.experimental import pallas as pl
from jax.experimental.pallas import tpu as pltpu
from jax.sharding import Mesh, PartitionSpec as P


EPS = 1e-06
PAIR = 2
PARTS = 4
KEPT = 2
f32, bf16 = jnp.float32, jnp.bfloat16


def row_of(values, index):
    here = lax.broadcasted_iota(jnp.int32, values.shape, 0) == index
    return jnp.sum(jnp.where(here, values, 0.0), axis=0, keepdims=True)


def dot_t(a, b):
    return lax.dot_general(a, b, (((1,), (1,)), ((), ())), preferred_element_type=f32)


def stage_kernel(
    x_hbm, gain_hbm, write_hbm, decay_hbm, rate_hbm, head_gain_hbm, *refs
):
    weights, (blocks_hbm, own_ref, x_ref, misc_ref), scratch = refs[:5], refs[5:9], refs[9:]
    half_ref, gain_ref, write_ref, decay_ref, rate_ref, head_gain_ref, sems = scratch
    half = blocks_hbm.shape[1]
    heads = blocks_hbm.shape[0] // (2 * PAIR)
    cols = blocks_hbm.shape[2]
    my_zh, my_za = lax.axis_index("zh"), lax.axis_index("za")
    my_z, my_y, my_h = my_zh * 2 + my_za, lax.axis_index("y"), lax.axis_index("h")
    here = pl.ds(pl.multiple_of(my_z * (PAIR * cols), PAIR * cols), PAIR * cols)
    moves = [(x_hbm, x_ref)] + [(ref, own_ref.at[m]) for m, ref in enumerate(weights)]
    moves += [
        (gain_hbm, gain_ref),
        (write_hbm.at[:, here], write_ref),
        (decay_hbm.at[:, here], decay_ref),
        (rate_hbm, rate_ref),
        (head_gain_hbm, head_gain_ref),
    ]
    copies = [pltpu.make_async_copy(a, b, sems.at[i]) for i, (a, b) in enumerate(moves)]
    for copy in copies:
        copy.start()
    copies[0].wait()
    for place in range(PAIR):
        rows = x_ref[place * half : (place + 1) * half, :]
        for head in range(heads):
            half_ref[place * heads + head] = rows
    spreads = [
        pltpu.make_async_copy(
            half_ref,
            blocks_hbm.at[pl.ds(plane * PAIR * heads, PAIR * heads)],
            sems.at[len(moves) + plane],
        )
        for plane in range(2)
    ]
    for copy in spreads:
        copy.start()
    for copy in copies[1:]:
        copy.wait()
    gains = gain_ref[...].astype(f32)
    lines = [
        row_of(gains, (my_zh * 2 + plane) * PAIR + place)
        for plane in (my_za, 1 - my_za)
        for place in (my_y, 1 - my_y)
    ]
    lines.append(head_gain_ref[...].astype(f32))
    rates = rate_ref[...]
    lane = lax.broadcasted_iota(jnp.int32, rates.shape, 1)
    rate = jnp.sum(jnp.where(lane == my_h, rates, 0.0), axis=1, keepdims=True)
    lines.append(jnp.broadcast_to(rate, (1, cols)))
    for ref in (write_ref, decay_ref):
        row = row_of(ref[...].astype(f32), my_h)
        low, high = row[:, :cols], row[:, cols:]
        lines.append(jnp.where(my_y == 0, low, high))
        lines.append(jnp.where(my_y == 0, high, low))
    for i, line in enumerate(lines):
        misc_ref[i : i + 1, :] = line
    for copy in spreads:
        copy.wait()


def send_kernel(own_ref, other_ref, far_ref):
    theirs = (1 - lax.axis_index("za")) * KEPT
    for i, ref in enumerate((own_ref, other_ref)):
        for m in range(KEPT):
            far_ref[i * KEPT + m] = ref[theirs + m]


def load_kernel(state_hbm, state_ref, sem):
    copy = pltpu.make_async_copy(state_hbm, state_ref, sem)
    copy.start()
    copy.wait()


def project_kernel(got_ref, own_ref, other_ref, far_ref, misc_ref, packed_ref):
    planes, half = packed_ref.shape[0], got_ref.shape[1]
    cols = got_ref.shape[2]
    heads = got_ref.shape[0] // (2 * PAIR)
    seqs = heads * half
    my_za, my_y = lax.axis_index("za"), lax.axis_index("y")
    squares, gained, small = None, [], None
    for p, plane in enumerate((my_za, 1 - my_za)):
        for i, place in enumerate((my_y, 1 - my_y)):
            x = got_ref[pl.ds((plane * PAIR + place) * heads, heads)]
            x = x.reshape(seqs, cols).astype(f32)
            line = p * PAIR + i
            g = (x * misc_ref[line : line + 1, :]).astype(bf16)
            gained.append(g)
            if p:
                continue
            squares = x * x if squares is None else squares + x * x
            line = lax.broadcasted_iota(jnp.int32, (128, cols), 0)
            write_row, decay_row = misc_ref[6 + i : 7 + i, :], misc_ref[8 + i : 9 + i, :]
            rows = jnp.where(line == 0, write_row, jnp.where(line == 1, decay_row, 0.0))
            term = dot_t(g, rows.astype(bf16))
            small = term if small is None else small + term
    mine = my_za * KEPT

    def beside(ref, start):
        return jnp.concatenate([ref[start + m] for m in range(KEPT)], axis=1)

    near = jnp.concatenate([beside(own_ref, mine), beside(other_ref, mine)], axis=0)
    far = jnp.concatenate([beside(far_ref, 0), beside(far_ref, KEPT)], axis=0)
    part = jnp.dot(jnp.concatenate(gained[:2], axis=1), near, preferred_element_type=f32)
    part = part + jnp.dot(jnp.concatenate(gained[2:], axis=1), far, preferred_element_type=f32)
    part = part.astype(bf16)
    for m in range(KEPT):
        piece = part[:, m * 128 : (m + 1) * 128].reshape(planes, half // 2, 2, 128)
        packed_ref[:, m * half // 2 : (m + 1) * half // 2] = piece
    total = jnp.sum(squares, axis=1, keepdims=True)
    lane = lax.broadcasted_iota(jnp.int32, small.shape, 1)
    small = jnp.where(lane == 2, total, small).T[:8]
    lane = lax.broadcasted_iota(jnp.int32, (1, 128), 1)
    for z in range(planes):
        start = z * half // 128 * 128
        line = small[:, start : start + 128]
        mine = lane // half == z % (128 // half)
        first = jnp.where(mine, line[0:1], pltpu.roll(line[1:2], 64, 1))
        tail = jnp.concatenate([first, line[2:3]], axis=0)
        packed_ref[z, KEPT * half // 2] = tail.astype(bf16)


def state_kernel(width, recv_ref, state_ref, misc_ref, spread_ref, updated_ref):
    planes, half, size = spread_ref.shape
    sums = [recv_ref[0].astype(f32), recv_ref[1].astype(f32)]
    for z in range(2, planes):
        sums[z % 2] = sums[z % 2] + recv_ref[z].astype(f32)
    tail = sums[0][KEPT * half // 2] + sums[1][KEPT * half // 2]
    my_z = lax.axis_index("zh") * 2 + lax.axis_index("za")
    tail = jnp.concatenate([tail, jnp.zeros((6, 128), f32)], axis=0)
    tail = pltpu.roll(tail, (128 - my_z % (128 // half) * half) % 128, 1)
    tail = jnp.concatenate([tail, pltpu.roll(tail, 64, 1)], axis=0).T[:half]
    sums = [part[: KEPT * half // 2].reshape(KEPT * half, size) for part in sums]
    row_scale = lax.rsqrt(tail[:, 1:2] / width + EPS)

    def scaled(value):
        return (value * row_scale).astype(bf16).astype(f32)

    query, key, value, gate = [
        scaled(sums[p][m * half : (m + 1) * half]) for p in range(2) for m in range(KEPT)
    ]
    pre = scaled(tail)
    query_norm = lax.rsqrt(jnp.sum(query * query, axis=1, keepdims=True) + EPS) * size**-0.5
    key_norm = lax.rsqrt(jnp.sum(key * key, axis=1, keepdims=True) + EPS)
    strength = jax.nn.sigmoid(pre[:, 0:1])
    rate = misc_ref[5:6, 0:1]
    decay_pre = pre[:, 8:9]
    softplus = jnp.maximum(decay_pre, 0.0) + jnp.log1p(jnp.exp(-jnp.abs(decay_pre)))
    factor = jnp.broadcast_to(jnp.exp(-rate * softplus), (half, size))
    query_t, key_t = query.T.astype(bf16), key.T.astype(bf16)
    match = jnp.sum(query * key, axis=1, keepdims=True) * query_norm * key_norm
    readouts = []
    for b in range(half):
        memory = state_ref[b]
        key_col = jnp.broadcast_to(key_t[:, b : b + 1], (size, size)).astype(f32)
        query_col = jnp.broadcast_to(query_t[:, b : b + 1], (size, size)).astype(f32)
        one = slice(b, b + 1)
        recalled = jnp.sum(memory * key_col, axis=0, keepdims=True) * key_norm[one]
        asked = jnp.sum(memory * query_col, axis=0, keepdims=True) * query_norm[one]
        fade = factor[one]
        correction = strength[one] * (value[one] - fade * recalled)
        updated_ref[b] = fade * memory + key_col * (key_norm[one] * correction)
        readouts.append(fade * asked + match[one] * correction)
    readout = jnp.concatenate(readouts, axis=0)
    scaling = lax.rsqrt(jnp.mean(readout * readout, axis=1, keepdims=True) + EPS)
    silu = gate / (1.0 + jnp.exp(-gate))
    gated = (scaling * readout * misc_ref[4:5, :] * silu).astype(bf16)
    for z in range(planes):
        spread_ref[z] = gated


def output_kernel(gated_ref, own_ref, other_ref, outs_ref):
    planes, half, size = gated_ref.shape
    my_y = lax.axis_index("y")
    gated = gated_ref[...].reshape(planes * half, size)
    for place, ref in ((my_y, own_ref), (1 - my_y, other_ref)):
        term = dot_t(gated, ref[PARTS]).astype(bf16)
        outs_ref[pl.ds(place * planes, planes)] = term.reshape(planes, half, -1)


def final_kernel(terms_ref, x_ref, updated_ref, out_hbm, state_hbm, out_ref, sems):
    half = terms_ref.shape[1]
    heads = terms_ref.shape[0] // PAIR
    state_copy = pltpu.make_async_copy(updated_ref, state_hbm, sems.at[0])
    state_copy.start()
    for place in range(PAIR):
        where = slice(place * half, (place + 1) * half)
        total = x_ref[where, :].astype(f32)
        for head in range(heads):
            total = total + terms_ref[place * heads + head].astype(f32)
        out_ref[where, :] = total.astype(bf16)
    out_copy = pltpu.make_async_copy(out_ref, out_hbm, sems.at[1])
    out_copy.start()
    state_copy.wait()
    out_copy.wait()


def per_device(
    stream,
    norm_gain,
    query_weight,
    key_weight,
    value_weight,
    gate_weight,
    write_weight,
    decay_weight,
    decay_rate,
    head_gain,
    out_weight,
    state,
):
    planes = lax.axis_size(("zh", "za"))
    heads = lax.axis_size("h")
    rows, cols = stream.shape
    half = rows // PAIR
    size = head_gain.shape[0]
    vmem, anywhere = pl.BlockSpec(memory_space=pltpu.VMEM), pl.BlockSpec(memory_space=pl.ANY)
    kept, plain = pltpu.VMEM, jax.ShapeDtypeStruct

    def call(kernel, outs, *args):
        args = [pltpu.with_memory_space_constraint(arg, pltpu.VMEM) for arg in args]
        specs = jax.tree.map(lambda _: vmem, outs)
        return pl.pallas_call(
            kernel, out_shape=outs, in_specs=[vmem] * len(args), out_specs=specs
        )(*args)

    whole = (norm_gain.reshape(-1, cols), write_weight.T, decay_weight.T)
    whole += (decay_rate.reshape(1, -1), head_gain.reshape(1, -1))
    blocks, own, x, misc = pl.pallas_call(
        stage_kernel,
        out_shape=(
            plain((2 * PAIR * heads, half, cols), bf16),
            kept((PARTS + 1, cols, size), bf16),
            kept((rows, cols), bf16),
            kept((16, cols), f32),
        ),
        in_specs=[anywhere] * 11,
        out_specs=(anywhere, vmem, vmem, vmem),
        scratch_shapes=[
            pltpu.VMEM((PAIR * heads, half, cols), bf16),
            pltpu.VMEM(whole[0].shape, bf16),
            pltpu.VMEM((heads, PAIR * cols), bf16),
            pltpu.VMEM((heads, PAIR * cols), bf16),
            pltpu.VMEM(whole[3].shape, f32),
            pltpu.VMEM(whole[4].shape, bf16),
            pltpu.SemaphoreType.DMA((13,)),
        ],
    )(stream, *whole, query_weight, key_weight, value_weight, gate_weight, out_weight)
    other = lax.ppermute(own, "y", [(0, 1), (1, 0)])
    far = call(send_kernel, kept((PAIR * KEPT, cols, size), bf16), own, other)
    far = lax.ppermute(far, "za", [(0, 1), (1, 0)])
    memory = pl.pallas_call(
        load_kernel,
        out_shape=kept(state.shape, f32),
        in_specs=[anywhere],
        out_specs=vmem,
        scratch_shapes=[pltpu.SemaphoreType.DMA],
    )(state)
    got = lax.all_to_all(blocks, ("za", "y", "h"), 0, 0)
    packed = call(
        project_kernel,
        kept((planes, KEPT * half // 2 + 1, 2, size), bf16),
        got, own, other, far, misc,
    )
    recv = lax.all_to_all(packed, ("zh", "za"), 0, 0)
    spread, updated = call(
        lambda *refs: state_kernel(cols * PAIR * planes, *refs),
        (kept((planes, half, size), bf16), kept(state.shape, f32)),
        recv, memory, misc,
    )
    all_gated = lax.all_to_all(spread, ("zh", "za"), 0, 0)
    outs = call(output_kernel, kept((PAIR * planes, half, cols), bf16), all_gated, own, other)
    terms = lax.all_to_all(outs, ("y", "h"), 0, 0)
    last = [pltpu.with_memory_space_constraint(arg, pltpu.VMEM) for arg in (terms, x, updated)]
    return tuple(
        pl.pallas_call(
            final_kernel,
            out_shape=(plain((rows, cols), bf16), plain(state.shape, f32)),
            in_specs=[vmem] * 3,
            out_specs=(anywhere, anywhere),
            scratch_shapes=[pltpu.VMEM((rows, cols), bf16), pltpu.SemaphoreType.DMA((2,))],
        )(*last)
    )


def solution(mesh):
    heads = 16
    grid = Mesh(mesh.devices.reshape(-1, 2, PAIR, heads), ("zh", "za", "y", "h"))
    every = ("zh", "za", "y", "h")
    flat, cube, same = P(every, None), P(every, None, None), P()
    placed = (flat, same, flat, flat, flat, flat, same, same, same, same, flat, cube)
    return jax.shard_map(
        per_device, mesh=grid, in_specs=placed, out_specs=(flat, cube), check_vma=False
    )
```
